32 devices in a mesh: ep: 16 (over z, y, core), tp: 2 (over x).
Axes of the slice: x: 2, y: 2, z: 4, core: 2. Of those that a mesh axis runs over, the one named last changes fastest.
Arguments:
- tokens: bfloat16 [256, 2048], P('ep'), may hold values from -6 to 6
- recur_state: float32 [256, 8, 128, 128], P('ep', 'tp'), may hold values from -0.4 to 0.4
- attn_gain: float32 [2048], replicated, may hold values from 0.1 to 1.9
- query_weight: bfloat16 [2048, 1024], P(None, 'tp'), may hold values from -0.125 to 0.125
- key_weight: bfloat16 [2048, 1024], P(None, 'tp'), may hold values from -0.125 to 0.125
- value_weight: bfloat16 [2048, 1024], P(None, 'tp'), may hold values from -0.125 to 0.125
- outgate_weight: bfloat16 [2048, 1024], P(None, 'tp'), may hold values from -0.125 to 0.125
- beta_weight: bfloat16 [2048, 8], replicated, may hold values from -0.125 to 0.125
- decay_weight: bfloat16 [2048, 8], replicated, may hold values from -0.125 to 0.125
- decay_rate: float32 [8], replicated, may hold values from 0.05 to 2
- head_gain: float32 [128], replicated, may hold values from 0.1 to 1.9
- output_weight: bfloat16 [1024, 2048], P('tp'), may hold values from -0.1875 to 0.1875
- ffn_gain: float32 [2048], replicated, may hold values from 0.1 to 1.9
- routes: int32 [256, 2], P('ep'), may hold values from 0 to 3, all different within a row; in each aligned block of 16 rows (0 to 15, 16 to 31, ...) at most 16 rows name the same one
- route_weight: float32 [256, 2], P('ep'), may hold values from 0.2 to 1
- expert_gate: bfloat16 [16, 2048, 1024], P('ep', None, 'tp'), may hold values from -0.125 to 0.125
- expert_up: bfloat16 [16, 2048, 1024], P('ep', None, 'tp'), may hold values from -0.125 to 0.125
- expert_down: bfloat16 [16, 1024, 2048], P('ep', 'tp'), may hold values from -0.09375 to 0.09375
Outputs:
- mixed: bfloat16 [256, 2048], P('ep', 'tp')
- new_state: float32 [256, 8, 128, 128], P('ep', 'tp')
The draws below stay inside these ranges and needn't reach their ends.
Inputs may be any that keep to these rules, and one draw needn't show every extreme that they name: `routes`: each row names 2 different experts; in each aligned block of 16 rows no expert is named by more than 16 rows.
All inputs are finite; a program needn't handle non-finite values.
Results may differ from the reference program's by a relative error of at most 0.014.
Values may be sent and summed in bfloat16 or wider, within the bound.
No kernel may reach another device: no remote copies, remote signals or barrier semaphores. Data moves between devices by JAX's collectives and lax.ppermute only.
A program may use at most 64 MiB of HBM per device.

```python
import math
import jax
import jax.numpy as jnp
import numpy as np
from jax import lax

D = 2048
H = 8
HEAD = 128
FF_E = 4096
TOP = 2
SEQ_DEV = 16
TOKENS = 256
EXPERTS = 4
FF_PART = 1024
CAP = 16
N_EP = 16


def levels(key, shape, cuts, low, largest):
    def one(dim, shards_of):
        steps = jax.random.uniform(jax.random.fold_in(jax.random.fold_in(key, 6), dim), (shards_of,), jnp.float32, low / len(cuts), largest / len(cuts))
        return jnp.repeat(jnp.exp(steps), shape[dim] // shards_of).reshape((-1,) + (1,) * (len(shape) - dim - 1))

    level = one(*cuts[0])
    for cut in cuts[1:]:
        level = level * one(*cut)
    return level


def shared_out(rng, own, number, rows, count, top, reach, lean):
    order = jax.random.permutation(rng, count)
    crowded, ordinary = load_shares(count, rows * top, reach, lean, True), load_shares(count, rows * top, reach, lean, False)
    places = jnp.arange(count)

    def named(sizes, offset_by):
        used = int((sizes > 0).sum())
        fixed = max(1, used // 4)
        passed = fixed + (places - fixed + offset_by * (used - fixed)) % max(1, count - fixed)
        return jnp.zeros((count,), jnp.int32).at[order[jnp.where(places < fixed, places, passed)]].set(jnp.asarray(sizes, jnp.int32))

    sizes = jnp.where(number % 4 == 0, named(crowded, number // 4), named(ordinary, number - number // 4 - 1))
    mixed = jax.random.permutation(jax.random.fold_in(own, 3), count)
    donor, sink = mixed[0:count // 2 * 2:2], mixed[1:count // 2 * 2:2]
    room = jnp.minimum(sizes[donor] - 1, reach - sizes[sink]) // 2
    room = jnp.where((donor == order[0]) | (sink == order[0]) | (sizes[sink] == 0), 0, jnp.maximum(room, 0))
    passed = jax.random.randint(jax.random.fold_in(own, 4), (count // 2,), 0, 1 << 20) % (room + 1)
    sizes = sizes.at[donor].add(-passed).at[sink].add(passed)
    members = jnp.searchsorted(jnp.cumsum(sizes), jnp.arange(rows * top), side="right").astype(jnp.int32)
    listing = members.reshape(top, rows).T
    listing = listing[jax.random.permutation(jax.random.fold_in(own, 1), rows)]
    offset_by = jax.random.randint(jax.random.fold_in(own, 2), (rows, 1), 0, top)
    return jnp.take_along_axis(listing, (jnp.arange(top)[None, :] + offset_by) % top, axis=1)


def load_shares(amount, total, most, lean, full):
    loads = [(1 << 20) // math.isqrt(grade ** lean) + 1 for grade in range(1, amount + 1)]
    largest = most if full else min(most, max(-(-total // amount), total * loads[0] // sum(loads)))
    least = 1 if total - largest >= amount - 1 else 0
    counts, spare = [largest] + [least] * (amount - 1), total - largest - least * (amount - 1)
    while spare > 0:
        candidates = [i for i in range(1, amount) if counts[i] < largest] or [i for i in range(1, amount) if counts[i] < most]
        pool, budget = sum([loads[i] for i in candidates]), spare
        for i in candidates:
            extra = min(most - counts[i], max(1, budget * loads[i] // pool), spare)
            counts[i] = counts[i] + extra
            spare = spare - extra
    return np.array(counts)


def scatter_about(own_key, shape, width, limit, shards=(), kind=jnp.bfloat16):
    values = width * jax.random.normal(own_key, shape, jnp.float32)
    if shards:
        values = values * levels(own_key, shape, shards, -0.22, 0.18)
    return jnp.clip(values, -limit, limit).astype(kind)


def setup_inputs(seed: int = 0) -> dict:
    splits = jax.random.split(jax.random.key(seed), 19)
    tokens = scatter_about(splits[0], (TOKENS, D), 1.0, 6.0, ((0, 16),))
    recur_state = scatter_about(splits[1], (TOKENS, H, HEAD, HEAD), 0.05, 0.4, ((0, 16), (1, 2)), jnp.float32)
    attn_gain = jnp.clip(1.0 + 0.18 * jax.random.normal(splits[2], (D,), jnp.float32), 0.1, 1.9)
    query_weight = scatter_about(splits[3], (D, H * HEAD), D ** -0.5, 0.125, ((1, 2),))
    key_weight = scatter_about(splits[4], (D, H * HEAD), D ** -0.5, 0.125, ((1, 2),))
    value_weight = scatter_about(splits[5], (D, H * HEAD), D ** -0.5, 0.125, ((1, 2),))
    outgate_weight = scatter_about(splits[6], (D, H * HEAD), D ** -0.5, 0.125, ((1, 2),))
    beta_weight = scatter_about(splits[7], (D, H), D ** -0.5, 0.125)
    decay_weight = scatter_about(splits[8], (D, H), D ** -0.5, 0.125)
    decay_rate = jnp.clip(jnp.exp(jax.random.uniform(splits[9], (H,), jnp.float32, math.log(0.05), math.log(2.0))), 0.05, 2.0)
    head_gain = jnp.clip(1.0 + 0.18 * jax.random.normal(splits[10], (HEAD,), jnp.float32), 0.1, 1.9)
    output_weight = scatter_about(splits[11], (H * HEAD, D), (H * HEAD) ** -0.5, 0.1875, ((0, 2),))
    ffn_gain = jnp.clip(1.0 + 0.18 * jax.random.normal(splits[12], (D,), jnp.float32), 0.1, 1.9)
    routes_keys = jax.random.split(jax.random.fold_in(splits[13], 1), TOKENS // SEQ_DEV)
    routes_turns = jax.random.permutation(jax.random.fold_in(splits[13], 3), TOKENS // SEQ_DEV)
    routes = jax.vmap(lambda own, number: shared_out(jax.random.fold_in(splits[13], 2), own, number, SEQ_DEV, EXPERTS, TOP, CAP, 2))(routes_keys, routes_turns).reshape((TOKENS, TOP))
    route_weight = jnp.clip(jnp.exp(math.log(1.0) - 1.609438 * jax.random.uniform(splits[14], (TOKENS, TOP), jnp.float32) ** levels(splits[14], (TOKENS, TOP), ((0, 16),), -0.2, 0.2)), 0.2, 1.0)
    expert_gate = scatter_about(splits[15], (4 * EXPERTS, D, FF_PART), D ** -0.5, 0.125, ((0, 16), (2, 2)))
    expert_up = scatter_about(splits[16], (4 * EXPERTS, D, FF_PART), D ** -0.5, 0.125, ((0, 16), (2, 2)))
    expert_down = scatter_about(splits[17], (4 * EXPERTS, FF_PART, D), FF_E ** -0.5, 0.09375, ((0, 16), (1, 2)))
    return {"tokens": tokens, "recur_state": recur_state, "attn_gain": attn_gain, "query_weight": query_weight, "key_weight": key_weight, "value_weight": value_weight, "outgate_weight": outgate_weight, "beta_weight": beta_weight, "decay_weight": decay_weight, "decay_rate": decay_rate, "head_gain": head_gain, "output_weight": output_weight, "ffn_gain": ffn_gain, "routes": routes, "route_weight": route_weight, "expert_gate": expert_gate, "expert_up": expert_up, "expert_down": expert_down}


EPS = 1e-06

def rms_scale(values, gain):
    return values * lax.rsqrt(lax.optimization_barrier(jnp.mean(values * values, axis=-1, keepdims=True)) + EPS) * gain

def unit_rows(values):
    return values * lax.rsqrt(lax.optimization_barrier(jnp.sum(values * values, axis=-1, keepdims=True)) + EPS)

def slot_targets(group_routes, experts, capacity):
    flat = group_routes.reshape(-1)
    onehot = (flat[:, None] == jnp.arange(experts, dtype=jnp.int32)[None, :]).astype(jnp.int32)
    running = jnp.cumsum(onehot, axis=0)
    position = lax.optimization_barrier(jnp.sum(running * onehot, axis=1)) - 1
    return (flat * capacity + position).reshape(group_routes.shape).astype(jnp.int32)

def reference(tokens, recur_state, attn_gain, query_weight, key_weight, value_weight, outgate_weight, beta_weight, decay_weight, decay_rate, head_gain, output_weight, ffn_gain, routes, route_weight, expert_gate, expert_up, expert_down):
    f32 = jnp.float32
    bf16 = jnp.bfloat16
    highest = lax.Precision.HIGHEST
    normed = rms_scale(tokens.astype(f32), attn_gain).astype(bf16)
    qproj = jnp.dot(normed, query_weight, preferred_element_type=f32).astype(bf16)
    kproj = jnp.dot(normed, key_weight, preferred_element_type=f32).astype(bf16)
    vproj = jnp.dot(normed, value_weight, preferred_element_type=f32).astype(bf16)
    zproj = jnp.dot(normed, outgate_weight, preferred_element_type=f32).astype(bf16)
    strength = jax.nn.sigmoid(jnp.dot(normed, beta_weight, preferred_element_type=f32))
    fading = jnp.exp(-decay_rate * jax.nn.softplus(jnp.dot(normed, decay_weight, preferred_element_type=f32)))

    def split_heads(proj):
        return proj.astype(f32).reshape(TOKENS, H, HEAD)
    query = unit_rows(jax.nn.silu(split_heads(qproj))) * HEAD ** (-0.5)
    keyvec = unit_rows(jax.nn.silu(split_heads(kproj)))
    value = jax.nn.silu(split_heads(vproj))
    recall = jnp.einsum('thd,thde->the', keyvec, recur_state, precision=highest)
    written = (strength[..., None] * keyvec)[..., :, None] * (value - fading[..., None] * recall)[..., None, :]
    new_state = fading[..., None, None] * recur_state + written
    readout = jnp.einsum('thd,thde->the', query, new_state, precision=highest)
    headed = (rms_scale(readout, head_gain) * jax.nn.silu(split_heads(zproj))).reshape(TOKENS, H * HEAD).astype(bf16)
    branch = jnp.dot(headed, output_weight, preferred_element_type=f32).astype(bf16)
    resid = (tokens.astype(f32) + branch.astype(f32)).astype(bf16)
    ffn_in = rms_scale(resid.astype(f32), ffn_gain).astype(bf16)
    grouped = ffn_in.reshape(N_EP, SEQ_DEV, D)
    group_routes = routes.reshape(N_EP, SEQ_DEV, TOP)
    group_weight = route_weight.reshape(N_EP, SEQ_DEV, TOP)
    targets = jax.vmap(lambda block: slot_targets(block, EXPERTS, CAP))(group_routes)
    slot_ids = jnp.arange(EXPERTS * CAP, dtype=jnp.int32)
    select = jnp.any(targets[:, None, :, :] == slot_ids[None, :, None, None], axis=-1).astype(f32)
    buffers = jnp.einsum('gst,gtd->gsd', select, grouped.astype(f32), precision=highest).astype(bf16)
    per_expert = buffers.reshape(N_EP, EXPERTS, CAP, D).transpose(1, 0, 2, 3).reshape(EXPERTS, N_EP * CAP, D)
    gates = expert_gate.reshape(EXPERTS, 4, D, FF_PART)
    ups = expert_up.reshape(EXPERTS, 4, D, FF_PART)
    downs = expert_down.reshape(EXPERTS, 4, FF_PART, D)

    def run_expert(operands):
        rows, gate_set, up_set, down_set = operands
        total = jnp.zeros((rows.shape[0], D), f32)
        for slice_idx in range(4):
            gated = jnp.dot(rows, gate_set[slice_idx], preferred_element_type=f32)
            lifted = jnp.dot(rows, up_set[slice_idx], preferred_element_type=f32)
            hidden = (jax.nn.silu(gated) * lifted).astype(bf16)
            piece = lax.optimization_barrier(jnp.dot(hidden, down_set[slice_idx], preferred_element_type=f32).astype(bf16))
            total = total + piece.astype(f32)
        return total
    results = lax.map(run_expert, (per_expert, gates, ups, downs))
    results = results.reshape(EXPERTS, N_EP, CAP, D).transpose(1, 0, 2, 3).reshape(N_EP, EXPERTS * CAP, D)
    combine = jnp.zeros((N_EP, SEQ_DEV, EXPERTS * CAP), f32)
    for choice_idx in range(TOP):
        match = (targets[..., choice_idx, None] == slot_ids).astype(f32)
        combine = combine + group_weight[..., choice_idx, None] * match
    moe = jnp.einsum('gts,gsd->gtd', combine, results, precision=highest).reshape(TOKENS, D)
    mixed = (resid.astype(f32) + moe).astype(bf16)
    return (mixed, new_state)
```

```python
import jax
import jax.numpy as jnp
from jax import lax
from jax.sharding import Mesh, PartitionSpec as P

EPS = 1e-06
SLICES = 4
CORES = 2
LANES = 128
EP = ("outer", "mid", "core")
PLANE = ("mid", "tp")


def rms_scale(values, gain):
    return values * lax.rsqrt(jnp.mean(values * values, axis=-1, keepdims=True) + EPS) * gain


def unit_rows(values):
    return values * lax.rsqrt(jnp.sum(values * values, axis=-1, keepdims=True) + EPS)


def swap(value, axes, offset):
    size = lax.axis_size(axes)
    return lax.ppermute(value, axes, [(i, i ^ offset) for i in range(size)])


def columns(value, index, width):
    return lax.dynamic_slice_in_dim(value, index * width, width, 1)


def mixer(
    tokens,
    recur_state,
    attn_gain,
    query_weight,
    key_weight,
    value_weight,
    outgate_weight,
    beta_weight,
    decay_weight,
    decay_rate,
    head_gain,
    output_weight,
):
    f32 = jnp.float32
    bf16 = jnp.bfloat16
    highest = lax.Precision.HIGHEST
    seq_count = tokens.shape[0]
    heads_here = recur_state.shape[1]
    head_size = recur_state.shape[2]
    normed = rms_scale(tokens.astype(f32), attn_gain).astype(bf16)
    qproj = jnp.dot(normed, query_weight, preferred_element_type=f32).astype(bf16)
    kproj = jnp.dot(normed, key_weight, preferred_element_type=f32).astype(bf16)
    vproj = jnp.dot(normed, value_weight, preferred_element_type=f32).astype(bf16)
    zproj = jnp.dot(normed, outgate_weight, preferred_element_type=f32).astype(bf16)
    first_head = lax.axis_index("tp") * heads_here
    own_beta = lax.dynamic_slice_in_dim(beta_weight, first_head, heads_here, 1)
    own_decay = lax.dynamic_slice_in_dim(decay_weight, first_head, heads_here, 1)
    own_rate = lax.dynamic_slice_in_dim(decay_rate, first_head, heads_here, 0)
    strength = jax.nn.sigmoid(jnp.dot(normed, own_beta, preferred_element_type=f32))
    fading = jnp.exp(
        -own_rate * jax.nn.softplus(jnp.dot(normed, own_decay, preferred_element_type=f32))
    )

    def split_heads(proj):
        return proj.astype(f32).reshape(seq_count, heads_here, head_size)

    query = unit_rows(jax.nn.silu(split_heads(qproj))) * head_size ** (-0.5)
    keyvec = unit_rows(jax.nn.silu(split_heads(kproj)))
    value = jax.nn.silu(split_heads(vproj))
    recall = jnp.einsum("thd,thde->the", keyvec, recur_state, precision=highest)
    written = (strength[..., None] * keyvec)[..., :, None] * (value - fading[..., None] * recall)[
        ..., None, :
    ]
    new_state = fading[..., None, None] * recur_state + written
    readout = jnp.einsum("thd,thde->the", query, new_state, precision=highest)
    headed = (
        (rms_scale(readout, head_gain) * jax.nn.silu(split_heads(zproj)))
        .reshape(seq_count, heads_here * head_size)
        .astype(bf16)
    )
    return jnp.dot(headed, output_weight, preferred_element_type=f32), new_state


def local(
    tokens,
    recur_state,
    attn_gain,
    query_weight,
    key_weight,
    value_weight,
    outgate_weight,
    beta_weight,
    decay_weight,
    decay_rate,
    head_gain,
    output_weight,
    ffn_gain,
    routes,
    route_weight,
    expert_gate,
    expert_up,
    expert_down,
):
    f32 = jnp.float32
    bf16 = jnp.bfloat16
    rows, model_width = tokens.shape
    outer = lax.axis_size("outer")
    mid = lax.axis_size("mid")
    lanes = lax.axis_size("tp")
    lane_index = lax.axis_index("tp")
    expert_index = lax.axis_index("outer")
    width = model_width // lanes

    partial_out, new_state = mixer(
        tokens,
        recur_state,
        attn_gain,
        query_weight,
        key_weight,
        value_weight,
        outgate_weight,
        beta_weight,
        decay_weight,
        decay_rate,
        head_gain,
        output_weight,
    )
    branch = columns(partial_out, lane_index, width)
    for offset in range(1, lanes):
        piece = columns(partial_out, lane_index ^ offset, width).astype(bf16)
        branch = branch + swap(piece, "tp", offset).astype(f32)
    resid = (
        columns(tokens, lane_index, width).astype(f32) + branch.astype(bf16).astype(f32)
    ).astype(bf16)

    expert_ids = jnp.arange(outer, dtype=jnp.int32)
    spread = jnp.sum(
        jnp.where(routes[:, :, None] == expert_ids[None, None, :], route_weight[:, :, None], 0.0),
        axis=1,
    )
    high = spread.astype(bf16)
    middle = (spread - high.astype(f32)).astype(bf16)
    low = (spread - high.astype(f32) - middle.astype(f32)).astype(bf16)
    coded = jnp.concatenate([high, middle, low], axis=1)
    extra = -(-coded.shape[1] // LANES) * LANES
    coded = jnp.pad(coded, ((0, 0), (0, extra - coded.shape[1])))

    held = jnp.concatenate([resid, coded], axis=1)
    held = jnp.concatenate(
        [held] + [swap(held, "outer", offset) for offset in range(1, outer)], axis=0
    )
    arrived = [held] + [swap(held, PLANE, offset) for offset in range(1, mid * lanes)]
    bands = []
    for row_offset in range(mid):
        parts = arrived[row_offset * lanes : (row_offset + 1) * lanes]
        ordered = []
        for position in range(lanes):
            chosen = parts[0][:, :width]
            for offset in range(1, lanes):
                chosen = jnp.where(
                    (lane_index ^ offset) == position, parts[offset][:, :width], chosen
                )
            ordered.append(chosen)
        bands.append(jnp.concatenate(ordered + [parts[0][:, width:]], axis=1))
    gathered = jnp.concatenate(bands, axis=0)
    gathered = jnp.concatenate([gathered, swap(gathered, "core", 1)], axis=0)

    codes = gathered[:, model_width:].astype(f32)
    own_code = jnp.arange(extra, dtype=jnp.int32)
    own_code = (own_code % outer == expert_index) & (own_code < 3 * outer)
    row_weight = jnp.sum(jnp.where(own_code[None, :], codes, 0.0), axis=1, keepdims=True)
    ffn_in = rms_scale(gathered[:, :model_width].astype(f32), ffn_gain).astype(bf16)
    gated = jnp.dot(ffn_in, expert_gate[0], preferred_element_type=f32)
    lifted = jnp.dot(ffn_in, expert_up[0], preferred_element_type=f32)
    hidden = (jax.nn.silu(gated) * lifted).astype(bf16)
    terms = (jnp.dot(hidden, expert_down[0], preferred_element_type=f32) * row_weight).astype(bf16)

    half = terms.shape[0] // CORES
    terms = terms[:half].astype(f32) + swap(terms[half:], "core", 1).astype(f32)
    band = half // mid
    total = columns(terms[:band], lane_index, width)
    terms = terms.astype(bf16)
    for row_offset in range(mid):
        for offset in range(lanes):
            if row_offset or offset:
                piece = columns(
                    terms[row_offset * band : (row_offset + 1) * band], lane_index ^ offset, width
                )
                total = total + swap(piece, PLANE, row_offset * lanes + offset).astype(f32)
    terms = total.astype(bf16)
    moe = total[:rows]
    for offset in range(1, outer):
        moe = moe + swap(terms[offset * rows : (offset + 1) * rows], "outer", offset).astype(f32)
    mixed = (resid.astype(f32) + moe).astype(bf16)
    return (mixed, new_state)


def solution(mesh):
    groups, lanes = mesh.shape["ep"], mesh.shape["tp"]
    shape = (groups // SLICES, SLICES // CORES, CORES, lanes)
    inner = Mesh(mesh.devices.reshape(shape), EP + ("tp",))
    return jax.shard_map(
        local,
        mesh=inner,
        in_specs=(
            P(EP, None),
            P(EP, "tp", None, None),
            P(),
            P(None, "tp"),
            P(None, "tp"),
            P(None, "tp"),
            P(None, "tp"),
            P(),
            P(),
            P(),
            P(),
            P("tp", None),
            P(),
            P(EP, None),
            P(EP, None),
            P(EP, None, "tp"),
            P(EP, None, "tp"),
            P(EP, "tp", None),
        ),
        out_specs=(P(EP, "tp"), P(EP, "tp", None, None)),
        check_vma=False,
    )
```

```python
import functools

import jax
import jax.numpy as jnp
from jax import lax
from jax.experimental import pallas as pl
from jax.experimental.pallas import tpu as pltpu
from jax.sharding import Mesh, PartitionSpec as P


EPS = 1e-06
SLICES = 4
CORES = 2
FILL_FLOPS = 1 << 30
EP = ("outer", "mid", "core")
PLANE = ("mid", "tp")


def rms_scale(values, gain):
    return values * lax.rsqrt(jnp.mean(values * values, axis=-1, keepdims=True) + EPS) * gain


def unit_rows(values):
    return values * lax.rsqrt(jnp.sum(values * values, axis=-1, keepdims=True) + EPS)


def near(value):
    return pltpu.with_memory_space_constraint(value, pltpu.VMEM)


def far(value):
    return pltpu.with_memory_space_constraint(value, pltpu.HBM)


def swap(value, axes, offset):
    size = lax.axis_size(axes)
    return lax.ppermute(value, axes, [(i, i ^ offset) for i in range(size)])


def columns(value, index, width):
    return lax.dynamic_slice_in_dim(value, index * width, width, 1)


def split_two(value):
    high = value.astype(jnp.bfloat16)
    return [high, (value - high.astype(jnp.float32)).astype(jnp.bfloat16)]


def mixer_kernel(lanes, *refs):
    f32 = jnp.float32
    bf16 = jnp.bfloat16
    sources, refs = refs[:12], refs[12:]
    own_ref, sent_ref, key_ref, written_ref, fade_ref = refs[:5]
    targets, refs = refs[5:16], refs[16:]
    state_vmem, load_sem, state_sem = refs
    tokens_ref, gain_ref, beta_ref, decay_ref, rate_ref, head_gain_ref = targets[:6]
    _, _, _, _, output_vmem = targets[6:]
    rows, heads_here, head_size, _ = state_vmem.shape
    lane_index = lax.axis_index("tp")
    loads = [
        pltpu.make_async_copy(source, target, load_sem.at[place])
        for place, (source, target) in enumerate(zip(sources, targets))
    ]
    state_loads = [
        pltpu.make_async_copy(sources[11].at[:, head], state_vmem.at[:, head], state_sem.at[head])
        for head in range(heads_here)
    ]
    for copy in loads[:9] + state_loads + loads[9:]:
        copy.start()

    for copy in loads[:6]:
        copy.wait()
    normed = rms_scale(tokens_ref[...].astype(f32), gain_ref[...]).astype(bf16)
    across = (((1,), (1,)), ((), ()))
    strength = jax.nn.sigmoid(
        lax.dot_general(normed, beta_ref[...], across, preferred_element_type=f32)
    )
    softened = jax.nn.softplus(
        lax.dot_general(normed, decay_ref[...], across, preferred_element_type=f32)
    )
    fading = jnp.exp(-rate_ref[...] * softened)
    head_ids = lax.broadcasted_iota(jnp.int32, strength.shape, 1)

    def of_head(table, head):
        chosen = head_ids == lane_index * heads_here + head
        return jnp.sum(jnp.where(chosen, table, 0.0), axis=1, keepdims=True)

    def project(place):
        loads[place].wait()
        proj = jnp.dot(normed, targets[place][...], preferred_element_type=f32)
        return proj.astype(bf16).astype(f32)

    def lanes_of(head):
        return slice(head * head_size, (head + 1) * head_size)

    kproj = project(6)
    vproj = project(7)
    qproj = project(8)
    readouts = []
    for head in range(heads_here):
        keyvec = unit_rows(jax.nn.silu(kproj[:, lanes_of(head)]))
        query = unit_rows(jax.nn.silu(qproj[:, lanes_of(head)])) * head_size ** (-0.5)
        value = jax.nn.silu(vproj[:, lanes_of(head)])
        fade = of_head(fading, head)
        both = jnp.concatenate([keyvec, query], axis=0)
        left = jnp.concatenate(split_two(both), axis=0)
        left = jnp.concatenate([left, left], axis=1)
        row_ids = lax.rem(lax.broadcasted_iota(jnp.int32, both.shape, 0), rows)
        found = jnp.zeros(both.shape, f32)
        state_loads[head].wait()
        for row in range(0, rows, 2):
            block = jnp.concatenate([state_vmem[row, head], state_vmem[row + 1, head]], axis=1)
            right = jnp.concatenate(split_two(block), axis=0)
            seen = jnp.dot(left, right, preferred_element_type=f32)
            seen = seen[: 2 * rows] + seen[2 * rows :]
            found = jnp.where(row_ids == row, seen[:, :head_size], found)
            found = jnp.where(row_ids == row + 1, seen[:, head_size:], found)
        recall, asked = found[:rows], found[rows:]
        written = of_head(strength, head) * (value - fade * recall)
        overlap = jnp.sum(query * keyvec, axis=1, keepdims=True)
        readouts.append(fade * asked + overlap * written)
        key_ref[:, lanes_of(head)] = keyvec
        written_ref[:, lanes_of(head)] = written
        fade_ref[:, head : head + 1] = fade
    zproj = project(9)
    headed = jnp.concatenate(
        [
            (
                rms_scale(readouts[head], head_gain_ref[...])
                * jax.nn.silu(zproj[:, lanes_of(head)])
            ).astype(bf16)
            for head in range(heads_here)
        ],
        axis=1,
    )
    loads[10].wait()
    width = own_ref.shape[1]

    def part(position):
        start = pl.multiple_of(position * width, width)
        return jnp.dot(headed, output_vmem[:, pl.ds(start, width)], preferred_element_type=f32)

    for offset in range(1, lanes):
        sent_ref[(offset - 1) * rows : offset * rows, :] = part(lane_index ^ offset).astype(bf16)
    own_ref[...] = part(lane_index)


def mixer(
    tokens,
    recur_state,
    attn_gain,
    query_weight,
    key_weight,
    value_weight,
    outgate_weight,
    beta_weight,
    decay_weight,
    decay_rate,
    head_gain,
    output_weight,
):
    f32 = jnp.float32
    bf16 = jnp.bfloat16
    rows, model_width = tokens.shape
    heads_here, head_size = recur_state.shape[1:3]
    lanes = lax.axis_size("tp")
    width = model_width // lanes
    vmem = pl.BlockSpec(memory_space=pltpu.VMEM)
    hbm = pl.BlockSpec(memory_space=pltpu.HBM)
    inputs = (
        tokens,
        attn_gain[None],
        beta_weight.T,
        decay_weight.T,
        decay_rate[None],
        head_gain[None],
        key_weight,
        value_weight,
        query_weight,
        outgate_weight,
        output_weight,
    )
    return pl.pallas_call(
        functools.partial(mixer_kernel, lanes),
        out_shape=(
            pltpu.VMEM((rows, width), f32),
            pltpu.VMEM((rows * (lanes - 1), width), bf16),
            pltpu.VMEM((rows, heads_here * head_size), f32),
            pltpu.VMEM((rows, heads_here * head_size), f32),
            pltpu.VMEM((rows, heads_here), f32),
        ),
        in_specs=[hbm] * 12,
        out_specs=[vmem] * 5,
        scratch_shapes=[pltpu.VMEM(value.shape, value.dtype) for value in inputs]
        + [
            pltpu.VMEM(recur_state.shape, f32),
            pltpu.SemaphoreType.DMA((len(inputs),)),
            pltpu.SemaphoreType.DMA((heads_here,)),
        ],
        compiler_params=pltpu.CompilerParams(vmem_limit_bytes=20 << 20),
        name="mixer",
    )(*map(far, inputs + (recur_state,)))


def update_kernel(
    state_hbm, key_ref, written_ref, fade_ref, out_hbm, state_vmem, held, load_sem, sem
):
    rows, heads_here, head_size, _ = held.shape
    loads = [
        pltpu.make_async_copy(state_hbm.at[:, head], state_vmem.at[:, head], load_sem.at[head])
        for head in range(heads_here)
    ]
    copies = [
        pltpu.make_async_copy(held.at[:, head], out_hbm.at[:, head], sem.at[head])
        for head in range(heads_here)
    ]
    for copy in loads:
        copy.start()
    for head in range(heads_here):
        lanes = slice(head * head_size, (head + 1) * head_size)
        key_turned = key_ref[:, lanes].T
        written = written_ref[:, lanes]
        fade = fade_ref[:, head : head + 1]
        loads[head].wait()
        for row in range(rows):
            held[row, head] = (
                fade[row : row + 1, :] * state_vmem[row, head]
                + key_turned[:, row : row + 1] * written[row : row + 1, :]
            )
        copies[head].start()
    for copy in copies:
        copy.wait()


def update(state, keyvec, written, fade):
    vmem = pl.BlockSpec(memory_space=pltpu.VMEM)
    hbm = pl.BlockSpec(memory_space=pltpu.HBM)
    semaphores = pltpu.SemaphoreType.DMA((state.shape[1],))
    return pl.pallas_call(
        update_kernel,
        out_shape=pltpu.HBM(state.shape, state.dtype),
        in_specs=[hbm] + [vmem] * 3,
        out_specs=hbm,
        scratch_shapes=[pltpu.VMEM(state.shape, state.dtype)] * 2 + [semaphores] * 2,
        compiler_params=pltpu.CompilerParams(vmem_limit_bytes=12 << 20),
        cost_estimate=pl.CostEstimate(
            flops=FILL_FLOPS, transcendentals=0, bytes_accessed=8 * state.size
        ),
        name="update",
    )(far(state), *map(near, (keyvec, written, fade)))


def fetch_kernel(count, *refs):
    sources, targets, sem = refs[1 : 1 + count], refs[1 + count : 1 + 2 * count], refs[-1]
    copies = [
        pltpu.make_async_copy(source, target, sem.at[place])
        for place, (source, target) in enumerate(zip(sources, targets))
    ]
    for copy in copies:
        copy.start()
    for copy in copies:
        copy.wait()


def fetch(after, *arrays):
    vmem = pl.BlockSpec(memory_space=pltpu.VMEM)
    hbm = pl.BlockSpec(memory_space=pltpu.HBM)
    size = sum(value.size * value.dtype.itemsize for value in arrays)
    return pl.pallas_call(
        functools.partial(fetch_kernel, len(arrays)),
        out_shape=[pltpu.VMEM(value.shape, value.dtype) for value in arrays],
        in_specs=[vmem] + [hbm] * len(arrays),
        out_specs=[vmem] * len(arrays),
        scratch_shapes=[pltpu.SemaphoreType.DMA((len(arrays),))],
        compiler_params=pltpu.CompilerParams(vmem_limit_bytes=8 << 20),
        cost_estimate=pl.CostEstimate(
            flops=FILL_FLOPS, transcendentals=0, bytes_accessed=2 * size
        ),
        name="fetch",
    )(near(after), *map(far, arrays))


def expert_kernel(mid, lanes, *refs):
    f32 = jnp.float32
    bf16 = jnp.bfloat16
    pieces = mid * lanes
    arrived = refs[: CORES * pieces]
    gain_ref, gate_ref, up_ref, down_ref = refs[CORES * pieces : CORES * pieces + 4]
    outs = refs[CORES * pieces + 4 : CORES * pieces + 4 + CORES * pieces]
    ffn_vmem = refs[CORES * pieces + 4 + CORES * pieces]
    band = arrived[0].shape[0]
    model_width = ffn_vmem.shape[1]
    width = model_width // lanes
    lane_index = lax.axis_index("tp")

    def columns_of(offset):
        return pl.ds(pl.multiple_of((lane_index ^ offset) * width, width), width)

    for block in range(CORES * mid):
        rows = slice(block * band, (block + 1) * band)
        parts = arrived[block * lanes : (block + 1) * lanes]
        squares = 0.0
        for part in parts:
            value = part[...].astype(f32)
            squares = squares + jnp.sum(value * value, axis=-1, keepdims=True)
        scale = lax.rsqrt(squares / model_width + EPS)
        for offset, part in enumerate(parts):
            where = columns_of(offset)
            ffn_vmem[rows, where] = (part[...].astype(f32) * scale * gain_ref[:, where]).astype(
                bf16
            )
    ffn_in = ffn_vmem[...]
    gated = jnp.dot(ffn_in, gate_ref[0], preferred_element_type=f32)
    lifted = jnp.dot(ffn_in, up_ref[0], preferred_element_type=f32)
    hidden = (jax.nn.silu(gated) * lifted).astype(bf16)
    for offset in range(lanes):
        terms = jnp.dot(hidden, down_ref[0, :, columns_of(offset)], preferred_element_type=f32)
        for block in range(CORES * mid):
            out = outs[block * lanes + offset]
            out[...] = terms[block * band : (block + 1) * band].astype(out.dtype)


def expert_slice(arrived, ffn_gain, expert_gate, expert_up, expert_down):
    f32 = jnp.float32
    bf16 = jnp.bfloat16
    mid, lanes = lax.axis_size("mid"), lax.axis_size("tp")
    model_width = ffn_gain.shape[0]
    band = arrived[0].shape[0]
    vmem = pl.BlockSpec(memory_space=pltpu.VMEM)
    shape = (band, model_width // lanes)
    rows = CORES * mid * band
    return pl.pallas_call(
        functools.partial(expert_kernel, mid, lanes),
        out_shape=[pltpu.VMEM(shape, f32)] * (mid * lanes)
        + [pltpu.VMEM(shape, bf16)] * (mid * lanes),
        in_specs=[vmem] * (CORES * mid * lanes + 4),
        out_specs=[vmem] * (CORES * mid * lanes),
        scratch_shapes=[pltpu.VMEM((rows, model_width), bf16)],
        compiler_params=pltpu.CompilerParams(vmem_limit_bytes=24 << 20),
        name="experts",
    )(*map(near, (*arrived, ffn_gain[None], expert_gate, expert_up, expert_down)))


def local(
    tokens,
    recur_state,
    attn_gain,
    query_weight,
    key_weight,
    value_weight,
    outgate_weight,
    beta_weight,
    decay_weight,
    decay_rate,
    head_gain,
    output_weight,
    ffn_gain,
    routes,
    route_weight,
    expert_gate,
    expert_up,
    expert_down,
):
    f32 = jnp.float32
    bf16 = jnp.bfloat16
    rows, model_width = tokens.shape
    outer = lax.axis_size("outer")
    mid = lax.axis_size("mid")
    lanes = lax.axis_size("tp")
    lane_index = lax.axis_index("tp")
    expert_index = lax.axis_index("outer")
    width = model_width // lanes

    branch, sent, *memory = mixer(
        tokens,
        recur_state,
        attn_gain,
        query_weight,
        key_weight,
        value_weight,
        outgate_weight,
        beta_weight,
        decay_weight,
        decay_rate,
        head_gain,
        output_weight,
    )
    for offset in range(1, lanes):
        piece = sent[(offset - 1) * rows : offset * rows]
        branch = branch + swap(piece, "tp", offset).astype(f32)
    resid = (
        columns(tokens, lane_index, width).astype(f32) + branch.astype(bf16).astype(f32)
    ).astype(bf16)

    new_state = update(recur_state, *memory)

    def weight_of(offset):
        named = routes == expert_index ^ offset
        return jnp.sum(jnp.where(named, route_weight, 0.0), axis=1, keepdims=True)

    held = resid
    held = jnp.concatenate(
        [held] + [swap(held, "outer", offset) for offset in range(1, outer)], axis=0
    )
    arrived = [held] + [swap(held, PLANE, offset) for offset in range(1, mid * lanes)]
    arrived = arrived + [swap(piece, "core", 1) for piece in arrived]
    fetched = fetch(sent, expert_gate, expert_up, expert_down)
    terms = expert_slice(arrived, ffn_gain, *fetched)
    own, other = terms[: mid * lanes], terms[mid * lanes :]
    total = own[0] + swap(other[0], "core", 1).astype(f32)
    for offset in range(1, mid * lanes):
        piece = (own[offset] + swap(other[offset], "core", 1).astype(f32)).astype(bf16)
        total = total + swap(piece, PLANE, offset).astype(f32)
    pieces = total.astype(bf16)
    moe = total[:rows] * weight_of(0)
    for offset in range(1, outer):
        piece = swap(pieces[offset * rows : (offset + 1) * rows], "outer", offset)
        moe = moe + piece.astype(f32) * weight_of(offset)
    mixed = (resid.astype(f32) + moe).astype(bf16)
    return (mixed, new_state)


def solution(mesh):
    groups, lanes = mesh.shape["ep"], mesh.shape["tp"]
    shape = (groups // SLICES, SLICES // CORES, CORES, lanes)
    inner = Mesh(mesh.devices.reshape(shape), EP + ("tp",))
    return jax.shard_map(
        local,
        mesh=inner,
        in_specs=(
            P(EP, None),
            P(EP, "tp", None, None),
            P(),
            P(None, "tp"),
            P(None, "tp"),
            P(None, "tp"),
            P(None, "tp"),
            P(),
            P(),
            P(),
            P(),
            P("tp", None),
            P(),
            P(EP, None),
            P(EP, None),
            P(EP, None, "tp"),
            P(EP, None, "tp"),
            P(EP, "tp", None),
        ),
        out_specs=(P(EP, "tp"), P(EP, "tp", None, None)),
        check_vma=False,
    )
```

```python
import functools
import itertools

import jax
import jax.numpy as jnp
from jax import lax
from jax.experimental import pallas as pl
from jax.experimental.pallas import tpu as pltpu
from jax.sharding import Mesh, PartitionSpec as P


EPS = 1e-06
SLICES = 4
CORES = 2
FILL_FLOPS = 1 << 30
EP = ("outer", "mid", "core")
PLANE = ("mid", "core", "tp")


def rms_scale(values, gain):
    return values * lax.rsqrt(jnp.mean(values * values, axis=-1, keepdims=True) + EPS) * gain


def unit_rows(values):
    return values * lax.rsqrt(jnp.sum(values * values, axis=-1, keepdims=True) + EPS)


def near(value):
    return pltpu.with_memory_space_constraint(value, pltpu.VMEM)


def far(value):
    return pltpu.with_memory_space_constraint(value, pltpu.HBM)


def swap(value, axes, offset):
    size = lax.axis_size(axes)
    return lax.ppermute(value, axes, [(i, i ^ offset) for i in range(size)])


def columns(value, index, width):
    return lax.dynamic_slice_in_dim(value, index * width, width, 1)


def turned(slot, lanes):
    return {1: lanes, lanes: 1}.get(slot, slot)


def plane_swap(value, slot):
    mid, cores, lanes = map(lax.axis_size, PLANE)
    pairs = []
    for m, c, t in itertools.product(range(mid), range(cores), range(lanes)):
        offset = turned(slot, lanes) if c else slot
        target = ((m ^ offset // lanes) * cores + c) * lanes + (t ^ offset % lanes)
        pairs.append(((m * cores + c) * lanes + t, target))
    return lax.ppermute(value, PLANE, pairs)


def split_two(value):
    high = value.astype(jnp.bfloat16)
    return [high, (value - high.astype(jnp.float32)).astype(jnp.bfloat16)]


def mixer_kernel(lanes, *refs):
    f32 = jnp.float32
    bf16 = jnp.bfloat16
    sources, refs = refs[:12], refs[12:]
    own_ref, sent_ref, key_ref, written_ref, fade_ref = refs[:5]
    targets, refs = refs[5:16], refs[16:]
    state_vmem, load_sem, state_sem = refs
    tokens_ref, gain_ref, beta_ref, decay_ref, rate_ref, head_gain_ref = targets[:6]
    _, _, _, _, output_vmem = targets[6:]
    rows, heads_here, head_size, _ = state_vmem.shape
    lane_index = lax.axis_index("tp")
    loads = [
        pltpu.make_async_copy(source, target, load_sem.at[place])
        for place, (source, target) in enumerate(zip(sources, targets))
    ]
    state_loads = [
        pltpu.make_async_copy(sources[11].at[:, head], state_vmem.at[:, head], state_sem.at[head])
        for head in range(heads_here)
    ]
    for copy in loads[:9] + state_loads + loads[9:]:
        copy.start()

    for copy in loads[:6]:
        copy.wait()
    normed = rms_scale(tokens_ref[...].astype(f32), gain_ref[...]).astype(bf16)
    across = (((1,), (1,)), ((), ()))
    strength = jax.nn.sigmoid(
        lax.dot_general(normed, beta_ref[...], across, preferred_element_type=f32)
    )
    softened = jax.nn.softplus(
        lax.dot_general(normed, decay_ref[...], across, preferred_element_type=f32)
    )
    fading = jnp.exp(-rate_ref[...] * softened)
    head_ids = lax.broadcasted_iota(jnp.int32, strength.shape, 1)

    def of_head(table, head):
        chosen = head_ids == lane_index * heads_here + head
        return jnp.sum(jnp.where(chosen, table, 0.0), axis=1, keepdims=True)

    def project(place):
        loads[place].wait()
        proj = jnp.dot(normed, targets[place][...], preferred_element_type=f32)
        return proj.astype(bf16).astype(f32)

    def lanes_of(head):
        return slice(head * head_size, (head + 1) * head_size)

    kproj = project(6)
    vproj = project(7)
    qproj = project(8)
    readouts = []
    for head in range(heads_here):
        keyvec = unit_rows(jax.nn.silu(kproj[:, lanes_of(head)]))
        query = unit_rows(jax.nn.silu(qproj[:, lanes_of(head)])) * head_size ** (-0.5)
        value = jax.nn.silu(vproj[:, lanes_of(head)])
        fade = of_head(fading, head)
        both = jnp.concatenate([keyvec, query], axis=0)
        left = jnp.concatenate(split_two(both), axis=0)
        left = jnp.concatenate([left, left], axis=1)
        row_ids = lax.rem(lax.broadcasted_iota(jnp.int32, both.shape, 0), rows)
        found = jnp.zeros(both.shape, f32)
        state_loads[head].wait()
        for row in range(0, rows, 2):
            block = jnp.concatenate([state_vmem[row, head], state_vmem[row + 1, head]], axis=1)
            right = jnp.concatenate(split_two(block), axis=0)
            seen = jnp.dot(left, right, preferred_element_type=f32)
            seen = seen[: 2 * rows] + seen[2 * rows :]
            found = jnp.where(row_ids == row, seen[:, :head_size], found)
            found = jnp.where(row_ids == row + 1, seen[:, head_size:], found)
        recall, asked = found[:rows], found[rows:]
        written = of_head(strength, head) * (value - fade * recall)
        overlap = jnp.sum(query * keyvec, axis=1, keepdims=True)
        readouts.append(fade * asked + overlap * written)
        key_ref[:, lanes_of(head)] = keyvec
        written_ref[:, lanes_of(head)] = written
        fade_ref[:, head : head + 1] = fade
    zproj = project(9)
    headed = jnp.concatenate(
        [
            (
                rms_scale(readouts[head], head_gain_ref[...])
                * jax.nn.silu(zproj[:, lanes_of(head)])
            ).astype(bf16)
            for head in range(heads_here)
        ],
        axis=1,
    )
    loads[10].wait()
    width = own_ref.shape[1]

    def part(position):
        start = pl.multiple_of(position * width, width)
        return jnp.dot(headed, output_vmem[:, pl.ds(start, width)], preferred_element_type=f32)

    for offset in range(1, lanes):
        sent_ref[(offset - 1) * rows : offset * rows, :] = part(lane_index ^ offset).astype(bf16)
    own_ref[...] = part(lane_index)


def mixer(
    tokens,
    recur_state,
    attn_gain,
    query_weight,
    key_weight,
    value_weight,
    outgate_weight,
    beta_weight,
    decay_weight,
    decay_rate,
    head_gain,
    output_weight,
):
    f32 = jnp.float32
    bf16 = jnp.bfloat16
    rows, model_width = tokens.shape
    heads_here, head_size = recur_state.shape[1:3]
    lanes = lax.axis_size("tp")
    width = model_width // lanes
    vmem = pl.BlockSpec(memory_space=pltpu.VMEM)
    hbm = pl.BlockSpec(memory_space=pltpu.HBM)
    inputs = (
        tokens,
        attn_gain[None],
        beta_weight.T,
        decay_weight.T,
        decay_rate[None],
        head_gain[None],
        key_weight,
        value_weight,
        query_weight,
        outgate_weight,
        output_weight,
    )
    return pl.pallas_call(
        functools.partial(mixer_kernel, lanes),
        out_shape=(
            pltpu.VMEM((rows, width), f32),
            pltpu.VMEM((rows * (lanes - 1), width), bf16),
            pltpu.VMEM((rows, heads_here * head_size), f32),
            pltpu.VMEM((rows, heads_here * head_size), f32),
            pltpu.VMEM((rows, heads_here), f32),
        ),
        in_specs=[hbm] * 12,
        out_specs=[vmem] * 5,
        scratch_shapes=[pltpu.VMEM(value.shape, value.dtype) for value in inputs]
        + [
            pltpu.VMEM(recur_state.shape, f32),
            pltpu.SemaphoreType.DMA((len(inputs),)),
            pltpu.SemaphoreType.DMA((heads_here,)),
        ],
        compiler_params=pltpu.CompilerParams(vmem_limit_bytes=20 << 20),
        name="mixer",
    )(*map(far, inputs + (recur_state,)))


def update_kernel(
    state_hbm, key_ref, written_ref, fade_ref, out_hbm, state_vmem, held, load_sem, sem
):
    rows, heads_here, head_size, _ = held.shape
    loads = [
        pltpu.make_async_copy(state_hbm.at[:, head], state_vmem.at[:, head], load_sem.at[head])
        for head in range(heads_here)
    ]
    copies = [
        pltpu.make_async_copy(held.at[:, head], out_hbm.at[:, head], sem.at[head])
        for head in range(heads_here)
    ]
    for copy in loads:
        copy.start()
    for head in range(heads_here):
        lanes = slice(head * head_size, (head + 1) * head_size)
        key_turned = key_ref[:, lanes].T
        written = written_ref[:, lanes]
        fade = fade_ref[:, head : head + 1]
        loads[head].wait()
        for row in range(rows):
            held[row, head] = (
                fade[row : row + 1, :] * state_vmem[row, head]
                + key_turned[:, row : row + 1] * written[row : row + 1, :]
            )
        copies[head].start()
    for copy in copies:
        copy.wait()


def update(state, keyvec, written, fade):
    vmem = pl.BlockSpec(memory_space=pltpu.VMEM)
    hbm = pl.BlockSpec(memory_space=pltpu.HBM)
    semaphores = pltpu.SemaphoreType.DMA((state.shape[1],))
    return pl.pallas_call(
        update_kernel,
        out_shape=pltpu.HBM(state.shape, state.dtype),
        in_specs=[hbm] + [vmem] * 3,
        out_specs=hbm,
        scratch_shapes=[pltpu.VMEM(state.shape, state.dtype)] * 2 + [semaphores] * 2,
        compiler_params=pltpu.CompilerParams(vmem_limit_bytes=12 << 20),
        cost_estimate=pl.CostEstimate(
            flops=FILL_FLOPS, transcendentals=0, bytes_accessed=8 * state.size
        ),
        name="update",
    )(far(state), *map(near, (keyvec, written, fade)))


def fetch_kernel(count, *refs):
    sources, targets, sem = refs[1 : 1 + count], refs[1 + count : 1 + 2 * count], refs[-1]
    copies = [
        pltpu.make_async_copy(source, target, sem.at[place])
        for place, (source, target) in enumerate(zip(sources, targets))
    ]
    for copy in copies:
        copy.start()
    for copy in copies:
        copy.wait()


def fetch(after, *arrays):
    vmem = pl.BlockSpec(memory_space=pltpu.VMEM)
    hbm = pl.BlockSpec(memory_space=pltpu.HBM)
    size = sum(value.size * value.dtype.itemsize for value in arrays)
    return pl.pallas_call(
        functools.partial(fetch_kernel, len(arrays)),
        out_shape=[pltpu.VMEM(value.shape, value.dtype) for value in arrays],
        in_specs=[vmem] + [hbm] * len(arrays),
        out_specs=[vmem] * len(arrays),
        scratch_shapes=[pltpu.SemaphoreType.DMA((len(arrays),))],
        compiler_params=pltpu.CompilerParams(vmem_limit_bytes=8 << 20),
        cost_estimate=pl.CostEstimate(
            flops=FILL_FLOPS, transcendentals=0, bytes_accessed=2 * size
        ),
        name="fetch",
    )(near(after), *map(far, arrays))


def expert_kernel(mid, lanes, *refs):
    f32 = jnp.float32
    bf16 = jnp.bfloat16
    pieces = mid * lanes
    arrived = refs[: CORES * pieces]
    gain_ref, gate_ref, up_ref, down_ref = refs[CORES * pieces : CORES * pieces + 4]
    outs = refs[CORES * pieces + 4 : CORES * pieces + 4 + CORES * pieces]
    ffn_vmem = refs[CORES * pieces + 4 + CORES * pieces]
    band = arrived[0].shape[0]
    model_width = ffn_vmem.shape[1]
    width = model_width // lanes
    lane_index = lax.axis_index("tp")

    def columns_of(offset):
        return pl.ds(pl.multiple_of((lane_index ^ offset) * width, width), width)

    first_core = lax.axis_index("core") == 0

    def of_core(values, slot, mirrored):
        other = turned(slot, lanes)
        if other == slot:
            return values[slot][...]
        pair = (values[other], values[slot]) if mirrored else (values[slot], values[other])
        return jnp.where(first_core, pair[0][...], pair[1][...])

    for block in range(CORES * mid):
        rows = slice(block * band, (block + 1) * band)
        group, row_offset = divmod(block, mid)
        held = arrived[group * pieces : (group + 1) * pieces]
        parts = [of_core(held, row_offset * lanes + place, group == 1) for place in range(lanes)]
        squares = 0.0
        for part in parts:
            value = part.astype(f32)
            squares = squares + jnp.sum(value * value, axis=-1, keepdims=True)
        scale = lax.rsqrt(squares / model_width + EPS)
        for offset, part in enumerate(parts):
            where = columns_of(offset)
            ffn_vmem[rows, where] = (part.astype(f32) * scale * gain_ref[:, where]).astype(bf16)
    ffn_in = ffn_vmem[...]
    gated = jnp.dot(ffn_in, gate_ref[0], preferred_element_type=f32)
    lifted = jnp.dot(ffn_in, up_ref[0], preferred_element_type=f32)
    hidden = (jax.nn.silu(gated) * lifted).astype(bf16)
    terms = [
        jnp.dot(hidden, down_ref[0, :, columns_of(offset)], preferred_element_type=f32)
        for offset in range(lanes)
    ]
    for group in range(CORES):
        values = [
            terms[slot % lanes][(group * mid + slot // lanes) * band :][:band]
            for slot in range(pieces)
        ]
        for slot in range(pieces):
            out = outs[group * pieces + slot]
            out[...] = of_core(values, slot, group == 1).astype(out.dtype)


def expert_slice(arrived, ffn_gain, expert_gate, expert_up, expert_down):
    f32 = jnp.float32
    bf16 = jnp.bfloat16
    mid, lanes = lax.axis_size("mid"), lax.axis_size("tp")
    model_width = ffn_gain.shape[0]
    band = arrived[0].shape[0]
    vmem = pl.BlockSpec(memory_space=pltpu.VMEM)
    shape = (band, model_width // lanes)
    rows = CORES * mid * band
    return pl.pallas_call(
        functools.partial(expert_kernel, mid, lanes),
        out_shape=[pltpu.VMEM(shape, f32)] * (mid * lanes)
        + [pltpu.VMEM(shape, bf16)] * (mid * lanes),
        in_specs=[vmem] * (CORES * mid * lanes + 4),
        out_specs=[vmem] * (CORES * mid * lanes),
        scratch_shapes=[pltpu.VMEM((rows, model_width), bf16)],
        compiler_params=pltpu.CompilerParams(vmem_limit_bytes=24 << 20),
        name="experts",
    )(*map(near, (*arrived, ffn_gain[None], expert_gate, expert_up, expert_down)))


def local(
    tokens,
    recur_state,
    attn_gain,
    query_weight,
    key_weight,
    value_weight,
    outgate_weight,
    beta_weight,
    decay_weight,
    decay_rate,
    head_gain,
    output_weight,
    ffn_gain,
    routes,
    route_weight,
    expert_gate,
    expert_up,
    expert_down,
):
    f32 = jnp.float32
    bf16 = jnp.bfloat16
    rows, model_width = tokens.shape
    outer = lax.axis_size("outer")
    mid = lax.axis_size("mid")
    lanes = lax.axis_size("tp")
    lane_index = lax.axis_index("tp")
    expert_index = lax.axis_index("outer")
    width = model_width // lanes

    branch, sent, *memory = mixer(
        tokens,
        recur_state,
        attn_gain,
        query_weight,
        key_weight,
        value_weight,
        outgate_weight,
        beta_weight,
        decay_weight,
        decay_rate,
        head_gain,
        output_weight,
    )
    for offset in range(1, lanes):
        piece = sent[(offset - 1) * rows : offset * rows]
        branch = branch + swap(piece, "tp", offset).astype(f32)
    resid = (
        columns(tokens, lane_index, width).astype(f32) + branch.astype(bf16).astype(f32)
    ).astype(bf16)

    new_state = update(recur_state, *memory)

    def weight_of(offset):
        named = routes == expert_index ^ offset
        return jnp.sum(jnp.where(named, route_weight, 0.0), axis=1, keepdims=True)

    held = resid
    held = jnp.concatenate(
        [held] + [swap(held, "outer", offset) for offset in range(1, outer)], axis=0
    )
    arrived = [held] + [plane_swap(held, offset) for offset in range(1, mid * lanes)]
    arrived = arrived + [swap(piece, "core", 1) for piece in arrived]
    fetched = fetch(sent, expert_gate, expert_up)
    fetched += fetch(sent, expert_down)
    terms = expert_slice(arrived, ffn_gain, *fetched)
    own, other = terms[: mid * lanes], terms[mid * lanes :]
    total = own[0] + swap(other[0], "core", 1).astype(f32)
    for offset in range(1, mid * lanes):
        piece = (own[offset] + swap(other[offset], "core", 1).astype(f32)).astype(bf16)
        total = total + plane_swap(piece, offset).astype(f32)
    pieces = total.astype(bf16)
    moe = total[:rows] * weight_of(0)
    for offset in range(1, outer):
        piece = swap(pieces[offset * rows : (offset + 1) * rows], "outer", offset)
        moe = moe + piece.astype(f32) * weight_of(offset)
    mixed = (resid.astype(f32) + moe).astype(bf16)
    return (mixed, new_state)


def solution(mesh):
    groups, lanes = mesh.shape["ep"], mesh.shape["tp"]
    shape = (groups // SLICES, SLICES // CORES, CORES, lanes)
    inner = Mesh(mesh.devices.reshape(shape), EP + ("tp",))
    return jax.shard_map(
        local,
        mesh=inner,
        in_specs=(
            P(EP, None),
            P(EP, "tp", None, None),
            P(),
            P(None, "tp"),
            P(None, "tp"),
            P(None, "tp"),
            P(None, "tp"),
            P(),
            P(),
            P(),
            P(),
            P("tp", None),
            P(),
            P(EP, None),
            P(EP, None),
            P(EP, None, "tp"),
            P(EP, None, "tp"),
            P(EP, "tp", None),
        ),
        out_specs=(P(EP, "tp"), P(EP, "tp", None, None)),
        check_vma=False,
    )
```

```python
import functools
import itertools

import jax
import jax.numpy as jnp
from jax import lax
from jax.experimental import pallas as pl
from jax.experimental.pallas import tpu as pltpu
from jax.sharding import Mesh, PartitionSpec as P


EPS = 1e-06
SLICES = 4
CORES = 2
FILL_FLOPS = 1 << 30
EXPERT_VMEM = 24 << 20
EP = ("outer", "mid", "core")
PLANE = ("mid", "core", "tp")


def rms_scale(values, gain):
    return values * lax.rsqrt(jnp.mean(values * values, axis=-1, keepdims=True) + EPS) * gain


def unit_rows(values):
    return values * lax.rsqrt(jnp.sum(values * values, axis=-1, keepdims=True) + EPS)


def near(value):
    return pltpu.with_memory_space_constraint(value, pltpu.VMEM)


def far(value):
    return pltpu.with_memory_space_constraint(value, pltpu.HBM)


def swap(value, axes, offset):
    size = lax.axis_size(axes)
    return lax.ppermute(value, axes, [(i, i ^ offset) for i in range(size)])


def columns(value, index, width):
    return lax.dynamic_slice_in_dim(value, index * width, width, 1)


def turned(slot, lanes):
    return {1: lanes, lanes: 1}.get(slot, slot)


def plane_swap(value, slot):
    mid, cores, lanes = map(lax.axis_size, PLANE)
    pairs = []
    for m, c, t in itertools.product(range(mid), range(cores), range(lanes)):
        offset = turned(slot, lanes) if c else slot
        target = ((m ^ offset // lanes) * cores + c) * lanes + (t ^ offset % lanes)
        pairs.append(((m * cores + c) * lanes + t, target))
    return lax.ppermute(value, PLANE, pairs)


def home_swap(value, offset):
    outer, mid, cores = map(lax.axis_size, EP)
    pairs = []
    for o, m, c in itertools.product(range(outer), range(mid), range(cores)):
        target = ((o ^ offset) * mid + m) * cores + (c ^ 1)
        pairs.append(((o * mid + m) * cores + c, target))
    return lax.ppermute(value, EP, pairs)


def split_two(value):
    high = value.astype(jnp.bfloat16)
    return [high, (value - high.astype(jnp.float32)).astype(jnp.bfloat16)]


def mixer_kernel(lanes, *refs):
    f32 = jnp.float32
    bf16 = jnp.bfloat16
    sources, refs = refs[:12], refs[12:]
    own_ref, sent_ref, key_ref, written_ref, fade_ref = refs[:5]
    targets, refs = refs[5:16], refs[16:]
    state_vmem, load_sem, state_sem = refs
    tokens_ref, gain_ref, beta_ref, decay_ref, rate_ref, head_gain_ref = targets[:6]
    _, _, _, _, output_vmem = targets[6:]
    rows, heads_here, head_size, _ = state_vmem.shape
    lane_index = lax.axis_index("tp")
    loads = [
        pltpu.make_async_copy(source, target, load_sem.at[place])
        for place, (source, target) in enumerate(zip(sources, targets))
    ]
    state_loads = [
        pltpu.make_async_copy(sources[11].at[:, head], state_vmem.at[:, head], state_sem.at[head])
        for head in range(heads_here)
    ]
    for copy in loads[:9] + state_loads + loads[9:]:
        copy.start()

    for copy in loads[:6]:
        copy.wait()
    normed = rms_scale(tokens_ref[...].astype(f32), gain_ref[...]).astype(bf16)
    across = (((1,), (1,)), ((), ()))
    strength = jax.nn.sigmoid(
        lax.dot_general(normed, beta_ref[...], across, preferred_element_type=f32)
    )
    softened = jax.nn.softplus(
        lax.dot_general(normed, decay_ref[...], across, preferred_element_type=f32)
    )
    fading = jnp.exp(-rate_ref[...] * softened)
    head_ids = lax.broadcasted_iota(jnp.int32, strength.shape, 1)

    def of_head(table, head):
        chosen = head_ids == lane_index * heads_here + head
        return jnp.sum(jnp.where(chosen, table, 0.0), axis=1, keepdims=True)

    def project(place):
        loads[place].wait()
        proj = jnp.dot(normed, targets[place][...], preferred_element_type=f32)
        return proj.astype(bf16).astype(f32)

    def lanes_of(head):
        return slice(head * head_size, (head + 1) * head_size)

    kproj = project(6)
    vproj = project(7)
    qproj = project(8)
    readouts = []
    for head in range(heads_here):
        keyvec = unit_rows(jax.nn.silu(kproj[:, lanes_of(head)]))
        query = unit_rows(jax.nn.silu(qproj[:, lanes_of(head)])) * head_size ** (-0.5)
        value = jax.nn.silu(vproj[:, lanes_of(head)])
        fade = of_head(fading, head)
        both = jnp.concatenate([keyvec, query], axis=0)
        left = jnp.concatenate(split_two(both), axis=0)
        left = jnp.concatenate([left, left], axis=1)
        row_ids = lax.rem(lax.broadcasted_iota(jnp.int32, both.shape, 0), rows)
        found = jnp.zeros(both.shape, f32)
        state_loads[head].wait()
        for row in range(0, rows, 2):
            block = jnp.concatenate([state_vmem[row, head], state_vmem[row + 1, head]], axis=1)
            right = jnp.concatenate(split_two(block), axis=0)
            seen = jnp.dot(left, right, preferred_element_type=f32)
            seen = seen[: 2 * rows] + seen[2 * rows :]
            found = jnp.where(row_ids == row, seen[:, :head_size], found)
            found = jnp.where(row_ids == row + 1, seen[:, head_size:], found)
        recall, asked = found[:rows], found[rows:]
        written = of_head(strength, head) * (value - fade * recall)
        overlap = jnp.sum(query * keyvec, axis=1, keepdims=True)
        readouts.append(fade * asked + overlap * written)
        key_ref[:, lanes_of(head)] = keyvec
        written_ref[:, lanes_of(head)] = written
        fade_ref[:, head : head + 1] = fade
    zproj = project(9)
    headed = jnp.concatenate(
        [
            (
                rms_scale(readouts[head], head_gain_ref[...])
                * jax.nn.silu(zproj[:, lanes_of(head)])
            ).astype(bf16)
            for head in range(heads_here)
        ],
        axis=1,
    )
    loads[10].wait()
    width = own_ref.shape[1]

    def part(position):
        start = pl.multiple_of(position * width, width)
        return jnp.dot(headed, output_vmem[:, pl.ds(start, width)], preferred_element_type=f32)

    for offset in range(1, lanes):
        sent_ref[(offset - 1) * rows : offset * rows, :] = part(lane_index ^ offset).astype(bf16)
    own_ref[...] = part(lane_index)


def mixer(
    tokens,
    recur_state,
    attn_gain,
    query_weight,
    key_weight,
    value_weight,
    outgate_weight,
    beta_weight,
    decay_weight,
    decay_rate,
    head_gain,
    output_weight,
):
    f32 = jnp.float32
    bf16 = jnp.bfloat16
    rows, model_width = tokens.shape
    heads_here, head_size = recur_state.shape[1:3]
    lanes = lax.axis_size("tp")
    width = model_width // lanes
    vmem = pl.BlockSpec(memory_space=pltpu.VMEM)
    hbm = pl.BlockSpec(memory_space=pltpu.HBM)
    inputs = (
        tokens,
        attn_gain[None],
        beta_weight.T,
        decay_weight.T,
        decay_rate[None],
        head_gain[None],
        key_weight,
        value_weight,
        query_weight,
        outgate_weight,
        output_weight,
    )
    return pl.pallas_call(
        functools.partial(mixer_kernel, lanes),
        out_shape=(
            pltpu.VMEM((rows, width), f32),
            pltpu.VMEM((rows * (lanes - 1), width), bf16),
            pltpu.VMEM((rows, heads_here * head_size), f32),
            pltpu.VMEM((rows, heads_here * head_size), f32),
            pltpu.VMEM((rows, heads_here), f32),
        ),
        in_specs=[hbm] * 12,
        out_specs=[vmem] * 5,
        scratch_shapes=[pltpu.VMEM(value.shape, value.dtype) for value in inputs]
        + [
            pltpu.VMEM(recur_state.shape, f32),
            pltpu.SemaphoreType.DMA((len(inputs),)),
            pltpu.SemaphoreType.DMA((heads_here,)),
        ],
        compiler_params=pltpu.CompilerParams(vmem_limit_bytes=20 << 20),
        name="mixer",
    )(*map(far, inputs + (recur_state,)))


def update_kernel(
    state_hbm, key_ref, written_ref, fade_ref, out_hbm, state_vmem, held, load_sem, sem
):
    rows, heads_here, head_size, _ = held.shape
    loads = [
        pltpu.make_async_copy(state_hbm.at[:, head], state_vmem.at[:, head], load_sem.at[head])
        for head in range(heads_here)
    ]
    copies = [
        pltpu.make_async_copy(held.at[:, head], out_hbm.at[:, head], sem.at[head])
        for head in range(heads_here)
    ]
    for copy in loads:
        copy.start()
    for head in range(heads_here):
        lanes = slice(head * head_size, (head + 1) * head_size)
        key_turned = key_ref[:, lanes].T
        written = written_ref[:, lanes]
        fade = fade_ref[:, head : head + 1]
        loads[head].wait()
        for row in range(rows):
            held[row, head] = (
                fade[row : row + 1, :] * state_vmem[row, head]
                + key_turned[:, row : row + 1] * written[row : row + 1, :]
            )
        copies[head].start()
    for copy in copies:
        copy.wait()


def update(state, keyvec, written, fade):
    vmem = pl.BlockSpec(memory_space=pltpu.VMEM)
    hbm = pl.BlockSpec(memory_space=pltpu.HBM)
    semaphores = pltpu.SemaphoreType.DMA((state.shape[1],))
    return pl.pallas_call(
        update_kernel,
        out_shape=pltpu.HBM(state.shape, state.dtype),
        in_specs=[hbm] + [vmem] * 3,
        out_specs=hbm,
        scratch_shapes=[pltpu.VMEM(state.shape, state.dtype)] * 2 + [semaphores] * 2,
        compiler_params=pltpu.CompilerParams(vmem_limit_bytes=12 << 20),
        cost_estimate=pl.CostEstimate(
            flops=FILL_FLOPS, transcendentals=0, bytes_accessed=8 * state.size
        ),
        name="update",
    )(far(state), *map(near, (keyvec, written, fade)))


def fetch_kernel(count, *refs):
    sources, targets, sem = refs[1 : 1 + count], refs[1 + count : 1 + 2 * count], refs[-1]
    copies = [
        pltpu.make_async_copy(source, target, sem.at[place])
        for place, (source, target) in enumerate(zip(sources, targets))
    ]
    for copy in copies:
        copy.start()
    for copy in copies:
        copy.wait()


def fetch(after, *arrays):
    vmem = pl.BlockSpec(memory_space=pltpu.VMEM)
    hbm = pl.BlockSpec(memory_space=pltpu.HBM)
    size = sum(value.size * value.dtype.itemsize for value in arrays)
    return pl.pallas_call(
        functools.partial(fetch_kernel, len(arrays)),
        out_shape=[pltpu.VMEM(value.shape, value.dtype) for value in arrays],
        in_specs=[vmem] + [hbm] * len(arrays),
        out_specs=[vmem] * len(arrays),
        scratch_shapes=[pltpu.SemaphoreType.DMA((len(arrays),))],
        compiler_params=pltpu.CompilerParams(vmem_limit_bytes=8 << 20),
        cost_estimate=pl.CostEstimate(
            flops=FILL_FLOPS, transcendentals=0, bytes_accessed=2 * size
        ),
        name="fetch",
    )(near(after), *map(far, arrays))


def expert_kernel(mid, lanes, handed, *refs):
    f32 = jnp.float32
    bf16 = jnp.bfloat16
    pieces = mid * lanes
    arrived, refs = refs[:pieces], refs[pieces:]
    gain_ref, gate_ref, up_ref, down_ref = refs[:4]
    outs, ffn_vmem = refs[4:-1], refs[-1]
    band = arrived[0].shape[0]
    model_width = ffn_vmem.shape[1]
    width = model_width // lanes
    lane_index = lax.axis_index("tp")
    core = lax.axis_index("core")
    source_first = core == (1 if handed else 0)
    target_first = core == (0 if handed else 1)

    def columns_of(offset):
        return pl.ds(pl.multiple_of((lane_index ^ offset) * width, width), width)

    def of_core(values, slot, core_is_first):
        other = turned(slot, lanes)
        if other == slot:
            return values[slot][...]
        return jnp.where(core_is_first, values[slot][...], values[other][...])

    for row_offset in range(mid):
        rows = slice(row_offset * band, (row_offset + 1) * band)
        parts = [
            of_core(arrived, row_offset * lanes + place, source_first) for place in range(lanes)
        ]
        squares = 0.0
        for part in parts:
            value = part.astype(f32)
            squares = squares + jnp.sum(value * value, axis=-1, keepdims=True)
        scale = lax.rsqrt(squares / model_width + EPS)
        for offset, part in enumerate(parts):
            where = columns_of(offset)
            ffn_vmem[rows, where] = (part.astype(f32) * scale * gain_ref[:, where]).astype(bf16)
    ffn_in = ffn_vmem[...]
    gated = jnp.dot(ffn_in, gate_ref[0], preferred_element_type=f32)
    lifted = jnp.dot(ffn_in, up_ref[0], preferred_element_type=f32)
    hidden = (jax.nn.silu(gated) * lifted).astype(bf16)
    terms = [
        jnp.dot(hidden, down_ref[0, :, columns_of(offset)], preferred_element_type=f32)
        for offset in range(lanes)
    ]
    values = [terms[slot % lanes][slot // lanes * band :][:band] for slot in range(pieces)]
    for slot in range(pieces):
        value = of_core(values, slot, target_first).astype(outs[0].dtype)
        if handed:
            outs[slot][...] = value
        elif slot < pieces - 1:
            outs[0][slot * band : (slot + 1) * band, :] = value
        else:
            outs[1][...] = value


def expert_slice(arrived, handed, dtype, ffn_gain, expert_gate, expert_up, expert_down):
    mid, lanes = lax.axis_size("mid"), lax.axis_size("tp")
    model_width = ffn_gain.shape[0]
    band = arrived[0].shape[0]
    vmem = pl.BlockSpec(memory_space=pltpu.VMEM)
    groups = (1,) * (mid * lanes) if handed else (mid * lanes - 1, 1)
    return pl.pallas_call(
        functools.partial(expert_kernel, mid, lanes, handed),
        out_shape=[pltpu.VMEM((count * band, model_width // lanes), dtype) for count in groups],
        in_specs=[vmem] * (mid * lanes + 4),
        out_specs=[vmem] * len(groups),
        scratch_shapes=[pltpu.VMEM((mid * band, model_width), jnp.bfloat16)],
        compiler_params=pltpu.CompilerParams(vmem_limit_bytes=EXPERT_VMEM),
        cost_estimate=pl.CostEstimate(
            flops=FILL_FLOPS, transcendentals=0, bytes_accessed=4 * expert_gate.size
        ),
        name="experts",
    )(*map(near, (*arrived, ffn_gain[None], expert_gate, expert_up, expert_down)))


def local(
    tokens,
    recur_state,
    attn_gain,
    query_weight,
    key_weight,
    value_weight,
    outgate_weight,
    beta_weight,
    decay_weight,
    decay_rate,
    head_gain,
    output_weight,
    ffn_gain,
    routes,
    route_weight,
    expert_gate,
    expert_up,
    expert_down,
):
    f32 = jnp.float32
    bf16 = jnp.bfloat16
    rows, model_width = tokens.shape
    outer = lax.axis_size("outer")
    mid = lax.axis_size("mid")
    lanes = lax.axis_size("tp")
    lane_index = lax.axis_index("tp")
    expert_index = lax.axis_index("outer")
    width = model_width // lanes

    branch, sent, *memory = mixer(
        tokens,
        recur_state,
        attn_gain,
        query_weight,
        key_weight,
        value_weight,
        outgate_weight,
        beta_weight,
        decay_weight,
        decay_rate,
        head_gain,
        output_weight,
    )
    for offset in range(1, lanes):
        piece = sent[(offset - 1) * rows : offset * rows]
        branch = branch + swap(piece, "tp", offset).astype(f32)
    resid = (
        columns(tokens, lane_index, width).astype(f32) + branch.astype(bf16).astype(f32)
    ).astype(bf16)

    new_state = update(recur_state, *memory)

    def weight_of(offset):
        named = routes == expert_index ^ offset
        return jnp.sum(jnp.where(named, route_weight, 0.0), axis=1, keepdims=True)

    held = resid
    held = jnp.concatenate(
        [held] + [swap(held, "outer", offset) for offset in range(1, outer)], axis=0
    )
    arrived = [held] + [plane_swap(held, offset) for offset in range(1, mid * lanes)]
    handed = [swap(piece, "core", 1) for piece in arrived]
    fetched = fetch(sent, expert_gate, expert_up)
    fetched += fetch(sent, expert_down)
    given = expert_slice(arrived, False, bf16, ffn_gain, *fetched)
    kept = expert_slice(handed, True, f32, ffn_gain, *fetched)
    last = swap(given[1], "core", 1).astype(f32)
    rest = swap(given[0], "core", 1).astype(f32)
    given = jnp.split(rest, mid * lanes - 1) + [last]
    total = kept[0] + given[0]
    for slot in range(1, mid * lanes):
        piece = (kept[slot] + given[slot]).astype(bf16)
        total = total + plane_swap(piece, slot).astype(f32)
    pieces = total.astype(bf16)
    moe = 0.0
    for offset in range(outer):
        piece = home_swap(pieces[offset * rows : (offset + 1) * rows], offset)
        moe = moe + piece.astype(f32) * weight_of(offset)
    mixed = (resid.astype(f32) + moe).astype(bf16)
    return (mixed, new_state)


def solution(mesh):
    groups, lanes = mesh.shape["ep"], mesh.shape["tp"]
    shape = (groups // SLICES, SLICES // CORES, CORES, lanes)
    inner = Mesh(mesh.devices.reshape(shape), EP + ("tp",))
    return jax.shard_map(
        local,
        mesh=inner,
        in_specs=(
            P(EP, None),
            P(EP, "tp", None, None),
            P(),
            P(None, "tp"),
            P(None, "tp"),
            P(None, "tp"),
            P(None, "tp"),
            P(),
            P(),
            P(),
            P(),
            P("tp", None),
            P(),
            P(EP, None),
            P(EP, None),
            P(EP, None, "tp"),
            P(EP, None, "tp"),
            P(EP, "tp", None),
        ),
        out_specs=(P(EP, "tp"), P(EP, "tp", None, None)),
        check_vma=False,
    )
```
